32 devices in a mesh: sp: 16 (over z, y, x), tp: 2 (over core).
Axes of the slice: x: 2, y: 2, z: 4, core: 2. Of those that a mesh axis runs over, the one named last changes fastest.
Arguments:
- query_matrix: bfloat16 [4096, 2048], P('sp', 'tp'), may hold values from -6 to 6
- key_matrix: bfloat16 [4096, 2048], P('sp', 'tp'), may hold values from -6 to 6
- value_matrix: bfloat16 [4096, 2048], P('sp', 'tp'), may hold values from -6 to 6
- output_gate_logits: bfloat16 [4096, 2048], P('sp', 'tp'), may hold values from -6 to 6
- decay_preactivation: bfloat16 [4096, 2048], P('sp', 'tp'), may hold values from -3 to 12
- head_extra_decay: float32 [4096, 32], P('sp', 'tp'), may hold values from -0.7 to 0
- residual: bfloat16 [4096, 2048], P(('sp', 'tp')), may hold values from -6 to 6
- head_norm_gain: float32 [64], replicated, may hold values from 0.1 to 1.9
- output_projection_weight: bfloat16 [2048, 2048], P('tp'), may hold values from -0.125 to 0.125
- mixer_norm_gain: float32 [2048], replicated, may hold values from 0.1 to 1.9
- routes: int32 [4096, 2], P(('sp', 'tp')), may hold values from 0 to 15, all different within a row; in each aligned block of 128 rows (0 to 127, 128 to 255, ...) at most 32 rows name the same one
- routing_weight: float32 [4096, 2], P(('sp', 'tp')), may hold values from 0.2 to 1.5
- routed_gate_weight: bfloat16 [16, 2048, 1024], P('sp', None, 'tp'), may hold values from -0.125 to 0.125
- routed_up_weight: bfloat16 [16, 2048, 1024], P('sp', None, 'tp'), may hold values from -0.125 to 0.125
- routed_down_weight: bfloat16 [16, 1024, 2048], P('sp', 'tp'), may hold values from -0.1875 to 0.1875
- common_gate_weight: bfloat16 [2048, 512], replicated, may hold values from -0.125 to 0.125
- common_up_weight: bfloat16 [2048, 512], replicated, may hold values from -0.125 to 0.125
- common_down_weight: bfloat16 [512, 2048], replicated, may hold values from -0.25 to 0.25
- final_norm_gain: float32 [2048], replicated, may hold values from 0.1 to 1.9
Outputs:
- layer_out: bfloat16 [4096, 2048], P(('sp', 'tp'))
The draws below stay inside these ranges and needn't reach their ends.
Inputs may be any that keep to these rules, and one draw needn't show every extreme that they name: `routes`: each row names 2 different experts. In the rows of one device (aligned blocks of rows) no expert is named by more than 32 rows, a bound that some block reaches.
All inputs are finite; a program needn't handle non-finite values.
Results may differ from the reference program's by a relative error of at most 0.019.
Values may be sent and summed in bfloat16 or wider, within the bound.
A program may use at most 192 MiB of HBM per device.

```python
import math
import jax
import jax.numpy as jnp
import numpy as np
from jax import lax

D = 2048
HEAD_NUMBER = 32
KEY_HEAD_SIZE = 64
BLOCK_TOKENS = 64
FE = 1024
FS = 512
TOP_K = 2
TOK_DEV = 256
SEQUENCE_TOKENS = 4096
EXPERTS = 16
CAP = 32
N_SP = 16
N_TP = 2


def draw_decay_preactivation(key, part):
    head_key, fast_key, slow_key, device_key, noise_key = jax.random.split(key, 5)
    fast_share = 0.5
    fast_head = jax.random.uniform(head_key, (HEAD_NUMBER,), jnp.float32) < fast_share
    fast_level = jax.random.uniform(fast_key, (HEAD_NUMBER, KEY_HEAD_SIZE), jnp.float32, -0.5, 1.0)
    slow_level = math.log(SEQUENCE_TOKENS / 9.6) + jax.random.uniform(slow_key, (HEAD_NUMBER, KEY_HEAD_SIZE), jnp.float32, -0.7, 0.7)
    level = jnp.where(fast_head[:, None], fast_level, slow_level).reshape(1, HEAD_NUMBER * KEY_HEAD_SIZE)
    device_shift = jax.random.uniform(device_key, (SEQUENCE_TOKENS // TOK_DEV, 1), jnp.float32, -0.7, 0.7)
    device_shift = jnp.repeat(device_shift, TOK_DEV, axis=0, total_repeat_length=SEQUENCE_TOKENS)
    noise = 0.7 * jax.random.normal(noise_key, (SEQUENCE_TOKENS, HEAD_NUMBER * KEY_HEAD_SIZE), jnp.float32)
    return jnp.clip(level + device_shift + noise, -3.0, 12.0).astype(jnp.bfloat16)


def draw_head_extra_decay(key, part):
    place_key, dropout_random_key = jax.random.split(key)
    places = jax.random.randint(place_key, (8,), 0, SEQUENCE_TOKENS)
    removed_entries = jnp.any(jnp.arange(SEQUENCE_TOKENS)[:, None] == places[None, :], axis=1)
    spike_dropped = jax.random.uniform(dropout_random_key, (SEQUENCE_TOKENS, HEAD_NUMBER), jnp.float32, -0.7, -0.22)
    return jnp.where(removed_entries[:, None], spike_dropped, 0.0).astype(jnp.float32)


def steps_of(key, dims, pieces, least, top_value):
    factor_of = 1.0
    for position, shards_of in pieces:
        heights = jax.random.uniform(jax.random.fold_in(jax.random.fold_in(key, 6), position), (shards_of,), jnp.float32, least / len(pieces), top_value / len(pieces))
        factor_of = factor_of * jnp.repeat(jnp.exp(heights), dims[position] // shards_of).reshape((-1,) + (1,) * (len(dims) - 1 - position))
    return factor_of


def shared_out(key, own, number, rows, amount, top, most, lean):
    sequence = jax.random.permutation(key, amount)
    heavy_load, common = shares(amount, rows * top, most, lean, True), shares(amount, rows * top, most, lean, False)
    places = jnp.arange(amount)

    def named(lengths, turn):
        used = int((lengths > 0).sum())
        fixed = max(1, used // 4)
        shifted = fixed + (places - fixed + turn * (used - fixed)) % max(1, amount - fixed)
        return jnp.zeros((amount,), jnp.int32).at[sequence[jnp.where(places < fixed, places, shifted)]].set(jnp.asarray(lengths, jnp.int32))

    lengths = jnp.where(number % 4 == 0, named(heavy_load, number // 4), named(common, number - number // 4 - 1))
    mixed = jax.random.permutation(jax.random.fold_in(own, 3), amount)
    donor, receiver = mixed[0:amount // 2 * 2:2], mixed[1:amount // 2 * 2:2]
    room = jnp.minimum(lengths[donor] - 1, most - lengths[receiver]) // 2
    room = jnp.where((donor == sequence[0]) | (receiver == sequence[0]) | (lengths[receiver] == 0), 0, jnp.maximum(room, 0))
    shifted = jax.random.randint(jax.random.fold_in(own, 4), (amount // 2,), 0, 1 << 20) % (room + 1)
    lengths = lengths.at[donor].add(-shifted).at[receiver].add(shifted)
    labels = jnp.searchsorted(jnp.cumsum(lengths), jnp.arange(rows * top), side="right").astype(jnp.int32)
    grid = labels.reshape(top, rows).T
    grid = grid[jax.random.permutation(jax.random.fold_in(own, 1), rows)]
    turn = jax.random.randint(jax.random.fold_in(own, 2), (rows, 1), 0, top)
    return jnp.take_along_axis(grid, (jnp.arange(top)[None, :] + turn) % top, axis=1)


def shares(amount, total, bound, lean, full):
    portions = [(1 << 20) // math.isqrt(rank ** lean) + 1 for rank in range(1, amount + 1)]
    largest = bound if full else min(bound, max(-(-total // amount), total * portions[0] // sum(portions)))
    least = 1 if total - largest >= amount - 1 else 0
    given, spare = [largest] + [least] * (amount - 1), total - largest - least * (amount - 1)
    while spare > 0:
        free = [i for i in range(1, amount) if given[i] < largest] or [i for i in range(1, amount) if given[i] < bound]
        whole, budget = sum([portions[i] for i in free]), spare
        for i in free:
            addition = min(bound - given[i], max(1, budget * portions[i] // whole), spare)
            given[i] = given[i] + addition
            spare = spare - addition
    return np.array(given)


def bell_draw(stream_key, dims, width, bound, cuts=(), kind=jnp.bfloat16):
    entries = width * jax.random.normal(stream_key, dims, jnp.float32)
    if cuts:
        entries = entries * steps_of(stream_key, dims, cuts, -0.22, 0.18)
    return jnp.clip(entries, -bound, bound).astype(kind)


def setup_inputs(seed: int = 0) -> dict:
    streams_of = jax.random.split(jax.random.key(seed), 20)
    query_matrix = bell_draw(streams_of[0], (SEQUENCE_TOKENS, HEAD_NUMBER * KEY_HEAD_SIZE), 1.0, 6.0, ((0, 16), (1, 2)))
    key_matrix = bell_draw(streams_of[1], (SEQUENCE_TOKENS, HEAD_NUMBER * KEY_HEAD_SIZE), 1.0, 6.0, ((0, 16), (1, 2)))
    value_matrix = bell_draw(streams_of[2], (SEQUENCE_TOKENS, HEAD_NUMBER * KEY_HEAD_SIZE), 1.0, 6.0, ((0, 16), (1, 2)))
    output_gate_logits = bell_draw(streams_of[3], (SEQUENCE_TOKENS, HEAD_NUMBER * KEY_HEAD_SIZE), 1.0, 6.0, ((0, 16), (1, 2)))
    decay_preactivation = draw_decay_preactivation(jax.random.fold_in(streams_of[19], 71), 0)
    head_extra_decay = draw_head_extra_decay(jax.random.fold_in(streams_of[19], 71), 0)
    residual = bell_draw(streams_of[6], (SEQUENCE_TOKENS, D), 1.0, 6.0, ((0, 32),))
    head_norm_gain = jnp.clip(1.0 + 0.18 * jax.random.normal(streams_of[7], (KEY_HEAD_SIZE,), jnp.float32), 0.1, 1.9)
    output_projection_weight = bell_draw(streams_of[8], (HEAD_NUMBER * KEY_HEAD_SIZE, D), (HEAD_NUMBER * KEY_HEAD_SIZE) ** -0.5, 0.125, ((0, 2),))
    mixer_norm_gain = jnp.clip(1.0 + 0.18 * jax.random.normal(streams_of[9], (D,), jnp.float32), 0.1, 1.9)
    routes_keys = jax.random.split(jax.random.fold_in(streams_of[10], 1), SEQUENCE_TOKENS // (TOK_DEV // N_TP))
    routes_turns = jax.random.permutation(jax.random.fold_in(streams_of[10], 3), SEQUENCE_TOKENS // (TOK_DEV // N_TP))
    routes = jax.vmap(lambda own, number: shared_out(jax.random.fold_in(streams_of[10], 2), own, number, TOK_DEV // N_TP, EXPERTS, TOP_K, CAP, 1))(routes_keys, routes_turns).reshape((SEQUENCE_TOKENS, TOP_K))
    routing_weight = jnp.clip(0.2 + 1.3 * jax.random.uniform(streams_of[11], (SEQUENCE_TOKENS, TOP_K), jnp.float32) ** steps_of(streams_of[11], (SEQUENCE_TOKENS, TOP_K), ((0, 32),), -0.2, 0.2), 0.2, 1.5)
    routed_gate_weight = bell_draw(streams_of[12], (EXPERTS, D, FE), D ** -0.5, 0.125, ((0, 16), (2, 2)))
    routed_up_weight = bell_draw(streams_of[13], (EXPERTS, D, FE), D ** -0.5, 0.125, ((0, 16), (2, 2)))
    routed_down_weight = bell_draw(streams_of[14], (EXPERTS, FE, D), FE ** -0.5, 0.1875, ((0, 16), (1, 2)))
    common_gate_weight = bell_draw(streams_of[15], (D, FS), D ** -0.5, 0.125)
    common_up_weight = bell_draw(streams_of[16], (D, FS), D ** -0.5, 0.125)
    common_down_weight = bell_draw(streams_of[17], (FS, D), FS ** -0.5, 0.25)
    final_norm_gain = jnp.clip(1.0 + 0.18 * jax.random.normal(streams_of[18], (D,), jnp.float32), 0.1, 1.9)
    return {"query_matrix": query_matrix, "key_matrix": key_matrix, "value_matrix": value_matrix, "output_gate_logits": output_gate_logits, "decay_preactivation": decay_preactivation, "head_extra_decay": head_extra_decay, "residual": residual, "head_norm_gain": head_norm_gain, "output_projection_weight": output_projection_weight, "mixer_norm_gain": mixer_norm_gain, "routes": routes, "routing_weight": routing_weight, "routed_gate_weight": routed_gate_weight, "routed_up_weight": routed_up_weight, "routed_down_weight": routed_down_weight, "common_gate_weight": common_gate_weight, "common_up_weight": common_up_weight, "common_down_weight": common_down_weight, "final_norm_gain": final_norm_gain}


EPS = 1e-06
GATE_DIVISOR = 16.0

def round_half(values):
    return lax.optimization_barrier(values.astype(jnp.bfloat16)).astype(jnp.float32)

def layer_norm(values, gain):
    center = values - lax.optimization_barrier(jnp.mean(values, axis=-1, keepdims=True))
    spread = lax.optimization_barrier(jnp.mean(center * center, axis=-1, keepdims=True))
    return center * lax.rsqrt(spread + EPS) * gain

def prepare_inputs(blocked_queries, blocked_keys, blocked_decay, spike_block_decay):
    logarithm_decay = jax.nn.log_sigmoid(blocked_decay.astype(jnp.float32)).reshape(BLOCK_TOKENS, HEAD_NUMBER, KEY_HEAD_SIZE) / GATE_DIVISOR
    logarithm_decay = logarithm_decay + spike_block_decay[:, :, None]
    inside_block = jnp.cumsum(logarithm_decay, axis=0)
    query_float = blocked_queries.astype(jnp.float32).reshape(BLOCK_TOKENS, HEAD_NUMBER, KEY_HEAD_SIZE) * KEY_HEAD_SIZE ** (-0.5)
    key_float = blocked_keys.astype(jnp.float32).reshape(BLOCK_TOKENS, HEAD_NUMBER, KEY_HEAD_SIZE)
    return (inside_block, query_float, key_float)

def forward_block(left_state, fragments):
    blocked_queries, blocked_keys, blocked_values, blocked_decay, spike_block_decay = fragments
    inside_block, query_float, key_float = prepare_inputs(blocked_queries, blocked_keys, blocked_decay, spike_block_decay)
    value_f = blocked_values.astype(jnp.float32).reshape(BLOCK_TOKENS, HEAD_NUMBER, KEY_HEAD_SIZE)
    total = inside_block[-1]
    query_up = query_float * jnp.exp(inside_block)
    query_down = query_float * jnp.exp(-inside_block)
    key_up = key_float * jnp.exp(inside_block)
    key_down = key_float * jnp.exp(-inside_block)
    lower_mask = jnp.tril(jnp.ones((BLOCK_TOKENS, BLOCK_TOKENS), bool))
    ahead = jnp.einsum('ihc,jhc->hij', query_up, key_down)
    behind = jnp.einsum('ihc,jhc->hij', query_down, key_up)
    scores = jnp.where(lower_mask, ahead, 0.0) + jnp.where(lower_mask, 0.0, behind)
    block_out = jnp.einsum('hij,jhv->ihv', scores, value_f)
    block_out = block_out + jnp.einsum('ihc,hcv->ihv', query_up, left_state)
    key_end = key_float * jnp.exp(total[None] - inside_block)
    new_state = jnp.exp(total)[..., None] * left_state + jnp.einsum('jhc,jhv->hcv', key_end, value_f)
    return (new_state, block_out)

def backward_block(right_state, fragments):
    blocked_queries, blocked_keys, blocked_values, blocked_decay, spike_block_decay = fragments
    inside_block, query_float, key_float = prepare_inputs(blocked_queries, blocked_keys, blocked_decay, spike_block_decay)
    value_f = blocked_values.astype(jnp.float32).reshape(BLOCK_TOKENS, HEAD_NUMBER, KEY_HEAD_SIZE)
    total = inside_block[-1]
    query_tail = query_float * jnp.exp(total[None] - inside_block)
    block_out = jnp.einsum('ihc,hcv->ihv', query_tail, right_state)
    key_up = key_float * jnp.exp(inside_block)
    new_state = jnp.exp(total)[..., None] * right_state + jnp.einsum('jhc,jhv->hcv', key_up, value_f)
    return (new_state, block_out)

def reference(query_matrix, key_matrix, value_matrix, output_gate_logits, decay_preactivation, head_extra_decay, residual, head_norm_gain, output_projection_weight, mixer_norm_gain, routes, routing_weight, routed_gate_weight, routed_up_weight, routed_down_weight, common_gate_weight, common_up_weight, common_down_weight, final_norm_gain):
    token_count = query_matrix.shape[0]
    number_of_blocks = token_count // BLOCK_TOKENS
    fragments = (query_matrix.reshape(number_of_blocks, BLOCK_TOKENS, HEAD_NUMBER * KEY_HEAD_SIZE), key_matrix.reshape(number_of_blocks, BLOCK_TOKENS, HEAD_NUMBER * KEY_HEAD_SIZE), value_matrix.reshape(number_of_blocks, BLOCK_TOKENS, HEAD_NUMBER * KEY_HEAD_SIZE), decay_preactivation.reshape(number_of_blocks, BLOCK_TOKENS, HEAD_NUMBER * KEY_HEAD_SIZE), head_extra_decay.reshape(number_of_blocks, BLOCK_TOKENS, HEAD_NUMBER))
    zero_state = jnp.zeros((HEAD_NUMBER, KEY_HEAD_SIZE, KEY_HEAD_SIZE), jnp.float32)
    _, forward_out = lax.scan(forward_block, zero_state, fragments)
    _, backward_out = lax.scan(backward_block, zero_state, fragments, reverse=True)
    mixed = (forward_out + backward_out).reshape(token_count, HEAD_NUMBER, KEY_HEAD_SIZE)
    normed_heads = mixed * lax.rsqrt(lax.optimization_barrier(jnp.mean(mixed * mixed, axis=-1, keepdims=True)) + EPS) * head_norm_gain
    gated = (normed_heads.reshape(token_count, HEAD_NUMBER * KEY_HEAD_SIZE) * jax.nn.silu(output_gate_logits.astype(jnp.float32))).astype(jnp.bfloat16)
    group_width = HEAD_NUMBER * KEY_HEAD_SIZE // N_TP
    projected = jnp.zeros((token_count, D), jnp.float32)
    for group in range(N_TP):
        part_sum = jnp.dot(gated[:, group * group_width:(group + 1) * group_width], output_projection_weight[group * group_width:(group + 1) * group_width], preferred_element_type=jnp.float32)
        projected = projected + round_half(part_sum)
    normed = layer_norm(residual.astype(jnp.float32) + projected, mixer_norm_gain).astype(jnp.bfloat16)
    sources = N_SP * N_TP
    row_count = TOK_DEV // N_TP
    assigned = row_count * TOP_K
    flat_routes = routes.reshape(sources, assigned)
    member = (flat_routes[:, :, None] == jnp.arange(EXPERTS, dtype=jnp.int32)[None, None, :]).astype(jnp.int32)
    rank_in = lax.optimization_barrier(jnp.sum((jnp.cumsum(member, axis=1) - member) * member, axis=2))
    column = jnp.arange(sources, dtype=jnp.int32)[:, None] * CAP + rank_in
    token_index = jnp.arange(sources, dtype=jnp.int32)[:, None] * row_count + jnp.arange(assigned, dtype=jnp.int32)[None, :] // TOP_K
    token_table = jnp.zeros((EXPERTS, sources * CAP), jnp.int32).at[flat_routes, column].set(token_index)
    weight_table = jnp.zeros((EXPERTS, sources * CAP), jnp.float32).at[flat_routes, column].set(routing_weight.reshape(sources, assigned))
    half_width = FE // N_TP

    def per_expert(total, expert_pieces):
        tokens_here, weights_here, gate_here, up_here, down_here = expert_pieces
        picked = normed[tokens_here]
        gate_part = jnp.dot(picked, gate_here, preferred_element_type=jnp.float32)
        up_part = jnp.dot(picked, up_here, preferred_element_type=jnp.float32)
        inner = (jax.nn.silu(gate_part) * up_part).astype(jnp.bfloat16)
        expert_sum = jnp.zeros((picked.shape[0], D), jnp.float32)
        for group in range(N_TP):
            expert_sum = expert_sum + round_half(jnp.dot(inner[:, group * half_width:(group + 1) * half_width], down_here[group * half_width:(group + 1) * half_width], preferred_element_type=jnp.float32))
        expert_result = round_half(expert_sum)
        return (total.at[tokens_here].add(weights_here[:, None] * expert_result), None)
    routed, _ = lax.scan(per_expert, jnp.zeros((token_count, D), jnp.float32), (token_table, weight_table, routed_gate_weight, routed_up_weight, routed_down_weight))
    shared_gate_out = jnp.dot(normed, common_gate_weight, preferred_element_type=jnp.float32)
    shared_up_out = jnp.dot(normed, common_up_weight, preferred_element_type=jnp.float32)
    shared_inner = (jax.nn.silu(shared_gate_out) * shared_up_out).astype(jnp.bfloat16)
    feed = jnp.dot(shared_inner, common_down_weight, preferred_element_type=jnp.float32) + routed
    return layer_norm(normed.astype(jnp.float32) + feed, final_norm_gain).astype(jnp.bfloat16)
```

```python
import functools

import jax
import jax.numpy as jnp
from jax import lax
from jax.experimental import pallas as pl
from jax.experimental.pallas import tpu as pltpu
from jax.sharding import PartitionSpec as P

KEY_HEAD_SIZE = 64
BLOCK_TOKENS = 64
EPS = 1e-06
GATE_DIVISOR = 16.0
LANES = 128
PLANES = 4
CHUNKS = 2
COLUMNS = 512
NORM_ROWS = 16
MESH = pl.DeviceIdType.MESH
OVER = (((0,), (0,)), ((), ()))
APART = (((1,), (1,)), ((), ()))


def lane_half(rows):
    return lax.broadcasted_iota(jnp.int32, (rows, LANES), 1) < KEY_HEAD_SIZE


def layer_norm(values, gain):
    center = values - jnp.mean(values, axis=-1, keepdims=True)
    spread = jnp.mean(center * center, axis=-1, keepdims=True)
    return center * lax.rsqrt(spread + EPS) * gain


def three(values):
    high = values.astype(jnp.bfloat16)
    rest = values - high.astype(jnp.float32)
    middle = rest.astype(jnp.bfloat16)
    low = (rest - middle.astype(jnp.float32)).astype(jnp.bfloat16)
    return high, middle, low


def product(left, right, dims=(((1,), (0,)), ((), ()))):
    return lax.dot_general(left, right, dims, preferred_element_type=jnp.float32)


def remote(source, destination, send, recv, device):
    return pltpu.make_async_remote_copy(
        src_ref=source,
        dst_ref=destination,
        send_sem=send,
        recv_sem=recv,
        device_id=device,
        device_id_type=MESH,
    )


def repeat(begin, end, body):
    def step(i, c):
        body(i)
        return c

    lax.fori_loop(begin, end, step, 0)


def columns_of(i, width=COLUMNS):
    return pl.ds(pl.multiple_of(i * width, width), width)


def mixer_kernel(
    n,
    q_ref,
    k_ref,
    v_ref,
    logits_ref,
    decay_ref,
    extra_ref,
    residual_ref,
    gain_ref,
    norm_gain_ref,
    weight_hbm,
    out_ref,
    weight_ref,
    summed_ref,
    wide_ref,
    local_ref,
    state_ref,
    total_ref,
    arrived,
    totals,
    ordered,
    before_ref,
    outbound,
    entered,
    gated_ref,
    given,
    taken,
    kept,
    send_state,
    recv_state,
    send_total,
    recv_total,
    send_back,
    recv_back,
    load_sem,
    send_part,
    recv_part,
):
    me, core = lax.axis_index("sp"), lax.axis_index("tp")
    peer = {"tp": 1 - core}
    tokens, width = q_ref.shape
    heads = extra_ref.shape[0]
    pairs = width // LANES
    rows = width // n
    owners = LANES // rows
    block = BLOCK_TOKENS
    model = weight_ref.shape[1]
    load = pltpu.make_async_copy(weight_hbm, weight_ref, load_sem)
    load.start()
    barrier = pltpu.get_barrier_semaphore()

    def greet(off):
        pl.semaphore_signal(
            barrier, inc=1, device_id={"sp": lax.rem(me + off, n)}, device_id_type=MESH
        )

    repeat(1, n, greet)
    pl.semaphore_signal(barrier, inc=1, device_id=peer, device_id_type=MESH)

    def forth(to):
        first = remote(
            state_ref.at[pl.ds(pl.multiple_of(to * rows, rows), rows)],
            arrived.at[me],
            send_state.at[to],
            recv_state.at[me],
            {"sp": to},
        )
        second = remote(
            total_ref.at[to // owners],
            totals.at[me],
            send_total.at[to],
            recv_total.at[me],
            {"sp": to},
        )
        return first, second

    def forth_in(source):
        first = remote(
            state_ref.at[pl.ds(0, rows)],
            arrived.at[source],
            send_state.at[source],
            recv_state.at[source],
            {"sp": source},
        )
        second = remote(
            total_ref.at[0],
            totals.at[source],
            send_total.at[source],
            recv_total.at[source],
            {"sp": source},
        )
        return first, second

    def back(to):
        return remote(
            outbound.at[to],
            entered.at[pl.ds(pl.multiple_of(me * rows, rows), rows)],
            send_back.at[to],
            recv_back.at[me],
            {"sp": to},
        )

    def back_in(source):
        return remote(
            outbound.at[source],
            entered.at[pl.ds(pl.multiple_of(source * rows, rows), rows)],
            send_back.at[source],
            recv_back.at[source],
            {"sp": source},
        )

    triangle = (
        lax.broadcasted_iota(jnp.int32, (tokens, tokens), 1)
        <= lax.broadcasted_iota(jnp.int32, (tokens, tokens), 0)
    ).astype(jnp.bfloat16)
    few = lane_half(KEY_HEAD_SIZE)
    half = lane_half(tokens)
    top, low = slice(0, KEY_HEAD_SIZE), slice(KEY_HEAD_SIZE, LANES)

    def prepare(step):
        pair = lax.rem(step + me // owners, pairs)
        lanes = columns_of(pair, LANES)
        decay = decay_ref[:, lanes].astype(jnp.float32)
        logarithm = jnp.minimum(decay, 0.0) - jnp.log1p(jnp.exp(-jnp.abs(decay)))
        row = lax.broadcasted_iota(jnp.int32, (heads, LANES), 0)
        lane = lax.broadcasted_iota(jnp.int32, (heads, LANES), 1)
        chosen = (row == pair * (LANES // KEY_HEAD_SIZE) + lane // KEY_HEAD_SIZE).astype(
            jnp.bfloat16
        )
        extra = sum(product(piece, chosen, OVER) for piece in three(extra_ref[...]))
        logarithm = logarithm * (1.0 / GATE_DIVISOR) + extra
        summed = sum(product(triangle, piece) for piece in three(logarithm))
        total = summed[tokens - 1 : tokens]
        summed_ref[pair] = summed
        query = q_ref[:, lanes].astype(jnp.float32) * KEY_HEAD_SIZE ** (-0.5)
        key = k_ref[:, lanes].astype(jnp.float32)
        value = v_ref[:, lanes]
        grown, rest = jnp.exp(summed), jnp.exp(total - summed)
        wide_ref[pair, :, :LANES] = (query * grown).astype(jnp.bfloat16)
        wide_ref[pair, :, LANES:] = (query * rest).astype(jnp.bfloat16)
        left = product((key * rest).astype(jnp.bfloat16), value, OVER)
        right = product((key * grown).astype(jnp.bfloat16), value, OVER)
        first = jnp.where(few, left[top], pltpu.roll(right[top], KEY_HEAD_SIZE, 1))
        second = jnp.where(few, pltpu.roll(left[low], KEY_HEAD_SIZE, 1), right[low])
        begin = pl.multiple_of(pair * LANES, LANES)
        state_ref[pl.ds(begin, LANES)] = jnp.concatenate([first, second], axis=0).astype(
            jnp.bfloat16
        )
        total_ref[pair] = total

        @pl.when(step == 0)
        def _():
            pl.semaphore_wait(barrier, n)

        def start(j):
            to = pair * owners + j

            @pl.when(to != me)
            def _():
                for copy in forth(to):
                    copy.start()

        repeat(0, owners, start)

    def attend(pair):
        lanes = columns_of(pair, LANES)
        summed = summed_ref[pair]
        query = q_ref[:, lanes].astype(jnp.float32) * KEY_HEAD_SIZE ** (-0.5)
        key = k_ref[:, lanes].astype(jnp.float32)
        value = v_ref[:, lanes]
        small = lane_half(block)
        for place in range(tokens // block):
            begin, end = place * block, (place + 1) * block
            own = summed[begin:end]
            before = summed[begin - 1 : begin] if place else jnp.zeros((1, LANES), jnp.float32)
            after = summed[end - 1 : end]
            mine = query[begin:end]
            ups = mine * jnp.exp(own - before)
            tails = mine * jnp.exp(after - own)
            ups = jnp.concatenate([jnp.where(small, ups, 0.0), jnp.where(small, 0.0, ups)], axis=0)
            tails = jnp.concatenate(
                [jnp.where(small, tails, 0.0), jnp.where(small, 0.0, tails)], axis=0
            )
            key_left = key[:end] * jnp.exp(jnp.minimum(before - summed[:end], 64.0))
            key_right = key[begin:] * jnp.exp(jnp.minimum(summed[begin:] - after, 64.0))
            ahead = product(ups.astype(jnp.bfloat16), key_left.astype(jnp.bfloat16), APART)
            behind = product(tails.astype(jnp.bfloat16), key_right.astype(jnp.bfloat16), APART)

            def place_of(size):
                here = lax.broadcasted_iota(jnp.int32, (2 * block, size), 0)
                return jnp.where(here < block, here, here - block)

            there = lax.broadcasted_iota(jnp.int32, (2 * block, end), 1)
            ahead = jnp.where(there <= place_of(end) + begin, ahead, 0.0)
            there = lax.broadcasted_iota(jnp.int32, (2 * block, tokens - begin), 1)
            behind = jnp.where(there > place_of(tokens - begin), behind, 0.0)
            both = product(ahead.astype(jnp.bfloat16), value[:end]) + product(
                behind.astype(jnp.bfloat16), value[begin:]
            )
            local_ref[pair, begin:end] = jnp.where(small, both[:block], both[block:])

    def finish(pair):
        lanes = columns_of(pair, LANES)
        begin = pl.multiple_of(pair * LANES, LANES)
        state = entered[pl.ds(begin, LANES)].astype(jnp.float32)
        first, second = state[top], state[low]
        states = jnp.concatenate(
            [
                jnp.where(few, first, 0.0),
                jnp.where(few, 0.0, pltpu.roll(second, KEY_HEAD_SIZE, 1)),
                jnp.where(few, pltpu.roll(first, KEY_HEAD_SIZE, 1), 0.0),
                jnp.where(few, 0.0, second),
            ],
            axis=0,
        ).astype(jnp.bfloat16)
        mixed = local_ref[pair] + product(wide_ref[pair], states)
        squares = mixed * mixed
        one = jnp.sum(jnp.where(half, squares, 0.0), axis=1, keepdims=True)
        two = jnp.sum(jnp.where(half, 0.0, squares), axis=1, keepdims=True)
        scale = jnp.where(
            half, lax.rsqrt(one / KEY_HEAD_SIZE + EPS), lax.rsqrt(two / KEY_HEAD_SIZE + EPS)
        )
        gate = jax.nn.silu(logits_ref[:, lanes].astype(jnp.float32))
        gated_ref[:, lanes] = (mixed * scale * gain_ref[...] * gate).astype(jnp.bfloat16)

    repeat(0, pairs, prepare)
    repeat(0, pairs // 2, attend)
    mine = pl.ds(pl.multiple_of(me * rows, rows), rows)
    arrived[me] = state_ref[mine]
    totals[me] = total_ref[me // owners]

    def wait_forth(off):
        for copy in forth_in(lax.rem(me + off, n)):
            copy.wait_recv()

    repeat(1, n, wait_forth)
    ordered[...] = jnp.zeros_like(ordered)
    for k in range(n):
        ordered[k : k + 1] = totals[k]
    turned = pltpu.roll(ordered[...], lax.rem(LANES - lax.rem(me * rows, LANES), LANES), 1)
    weights = jnp.exp(turned.T)[:rows]
    carried = jnp.zeros((rows, LANES), jnp.float32)
    for k in range(n):
        before_ref[k] = carried
        if k < n - 1:
            carried = weights[:, k : k + 1] * carried + arrived[k].astype(jnp.float32)
    carried = jnp.zeros((rows, LANES), jnp.float32)
    first_half = lane_half(rows)
    for k in range(n - 1, -1, -1):
        outbound[k] = jnp.where(first_half, before_ref[k], carried).astype(jnp.bfloat16)
        if k:
            carried = weights[:, k : k + 1] * carried + arrived[k].astype(jnp.float32)

    repeat(1, n, lambda off: back(lax.rem(me + off, n)).start())
    entered[mine] = outbound[me]
    repeat(pairs // 2, pairs, attend)
    repeat(1, n, lambda off: back_in(lax.rem(me + off, n)).wait_recv())
    repeat(0, pairs, finish)
    load.wait()
    few_rows = tokens // 2
    theirs = pl.ds(pl.multiple_of((1 - core) * few_rows, few_rows), few_rows)
    ours = pl.ds(pl.multiple_of(core * few_rows, few_rows), few_rows)

    def trade(i):
        return remote(
            given.at[:, columns_of(i)],
            taken.at[:, columns_of(i)],
            send_part.at[i],
            recv_part.at[i],
            peer,
        )

    def project_theirs(i):
        given[:, columns_of(i)] = product(
            gated_ref[theirs, :], weight_ref[:, columns_of(i)]
        ).astype(jnp.bfloat16)
        trade(i).start()

    def project_ours(i):
        kept[:, columns_of(i)] = product(
            gated_ref[ours, :], weight_ref[:, columns_of(i)]
        ).astype(jnp.bfloat16)

    parts = model // COLUMNS
    repeat(0, parts, project_theirs)
    repeat(0, parts, project_ours)
    repeat(0, parts, lambda i: trade(i).wait_recv())

    def normalize(i):
        some = pl.ds(pl.multiple_of(i * NORM_ROWS, NORM_ROWS), NORM_ROWS)
        projected = kept[some].astype(jnp.float32) + taken[some].astype(jnp.float32)
        out_ref[some] = layer_norm(
            residual_ref[some].astype(jnp.float32) + projected, norm_gain_ref[...]
        ).astype(jnp.bfloat16)

    repeat(0, few_rows // NORM_ROWS, normalize)

    def sent(off):
        to = lax.rem(me + off, n)
        for copy in forth(to):
            copy.wait_send()
        back(to).wait_send()

    repeat(1, n, sent)
    repeat(0, parts, lambda i: trade(i).wait_send())


def mixer(query, key, value, logits, decay, extra, residual, gain, norm_gain, weight):
    n = lax.axis_size("sp")
    tokens, width = query.shape
    pairs, rows, model = width // LANES, width // n, weight.shape[1]
    half = (tokens // 2, model)
    vmem, anywhere = pl.BlockSpec(memory_space=pltpu.VMEM), pl.BlockSpec(memory_space=pl.ANY)
    each = pltpu.SemaphoreType.DMA((n,))
    parts = pltpu.SemaphoreType.DMA((model // COLUMNS,))
    return pl.pallas_call(
        functools.partial(mixer_kernel, n),
        in_specs=[vmem] * 9 + [anywhere],
        out_specs=vmem,
        out_shape=jax.ShapeDtypeStruct(half, jnp.bfloat16),
        scratch_shapes=[
            pltpu.VMEM(weight.shape, jnp.bfloat16),
            pltpu.VMEM((pairs, tokens, LANES), jnp.float32),
            pltpu.VMEM((pairs, tokens, 2 * LANES), jnp.bfloat16),
            pltpu.VMEM((pairs, tokens, LANES), jnp.float32),
            pltpu.VMEM((width, LANES), jnp.bfloat16),
            pltpu.VMEM((pairs, 1, LANES), jnp.float32),
            pltpu.VMEM((n, rows, LANES), jnp.bfloat16),
            pltpu.VMEM((n, 1, LANES), jnp.float32),
            pltpu.VMEM((LANES, LANES), jnp.float32),
            pltpu.VMEM((n, rows, LANES), jnp.float32),
            pltpu.VMEM((n, rows, LANES), jnp.bfloat16),
            pltpu.VMEM((width, LANES), jnp.bfloat16),
            pltpu.VMEM((tokens, width), jnp.bfloat16),
            pltpu.VMEM(half, jnp.bfloat16),
            pltpu.VMEM(half, jnp.bfloat16),
            pltpu.VMEM(half, jnp.bfloat16),
            each,
            each,
            each,
            each,
            each,
            each,
            pltpu.SemaphoreType.DMA(()),
            parts,
            parts,
        ],
        compiler_params=pltpu.CompilerParams(collective_id=0, has_side_effects=True),
        name="mixer",
    )(query, key, value, logits, decay, extra, residual, gain, norm_gain, weight)


def expert_kernel(
    n,
    normed_ref,
    routes_ref,
    routing_ref,
    gain_ref,
    gate_hbm,
    up_hbm,
    down_hbm,
    common_gate_hbm,
    common_up_hbm,
    common_down_hbm,
    out_ref,
    gate_ref,
    up_ref,
    down_ref,
    common_gate,
    common_up,
    common_down,
    meta,
    gathered,
    picked,
    rows_in,
    given,
    taken,
    kept,
    summed,
    returned,
    feed,
    load_sem,
    send_meta,
    recv_meta,
    send_line,
    recv_line,
    send_pick,
    recv_pick,
    copy_pick,
    send_share,
    recv_share,
    send_part,
    recv_part,
    send_back,
    recv_back,
):
    me, core = lax.axis_index("sp"), lax.axis_index("tp")
    peer = {"tp": 1 - core}
    members = n // PLANES
    plane, member = me // members, lax.rem(me, members)
    rows, width = normed_ref.shape
    capacity = returned.shape[1]
    slots = members * capacity
    inner = (plane > 0) & (plane < PLANES - 1)
    parts = width // COLUMNS
    chunk = rows // CHUNKS

    def source_at(k):
        low = plane < PLANES // 2
        one = jnp.where(low, plane + 1, plane - 1)
        two = jnp.where(low, 2 - 2 * plane, 7 - 2 * plane)
        three_ = jnp.where(low, PLANES - 1, 0)
        return jnp.where(k == 0, plane, jnp.where(k == 1, one, jnp.where(k == 2, two, three_)))

    loads = [
        pltpu.make_async_copy(common_gate_hbm, common_gate, load_sem.at[0]),
        pltpu.make_async_copy(common_up_hbm, common_up, load_sem.at[1]),
        pltpu.make_async_copy(common_down_hbm, common_down, load_sem.at[2]),
        pltpu.make_async_copy(gate_hbm, gate_ref, load_sem.at[3]),
        pltpu.make_async_copy(up_hbm, up_ref, load_sem.at[4]),
        pltpu.make_async_copy(down_hbm, down_ref, load_sem.at[5]),
    ]
    own = pltpu.make_async_copy(normed_ref, gathered.at[plane], load_sem.at[6])
    own.start()
    barrier = pltpu.get_barrier_semaphore()

    def greet(device):
        pl.semaphore_signal(barrier, inc=1, device_id=device, device_id_type=MESH)

    for off in range(1, PLANES):
        greet({"sp": lax.rem(plane + off, PLANES) * members + member})
    repeat(1, members, lambda q: greet({"sp": plane * members + lax.rem(member + q, members)}))
    greet(peer)
    for load in loads:
        load.start()
    expert = lax.broadcasted_iota(jnp.int32, (n, rows), 0)
    one = (expert == routes_ref[0:1]).astype(jnp.float32)
    two = (expert == routes_ref[1:2]).astype(jnp.float32)
    earlier = (
        lax.broadcasted_iota(jnp.int32, (rows, rows), 0)
        < lax.broadcasted_iota(jnp.int32, (rows, rows), 1)
    ).astype(jnp.bfloat16)
    rank = product((one + two).astype(jnp.bfloat16), earlier)
    place = (expert * capacity).astype(jnp.float32) + rank
    meta[plane] = jnp.zeros(meta.shape[1:], jnp.float32)
    meta[plane, 0:1] = jnp.sum(one * place, axis=0, keepdims=True)
    meta[plane, 1:2] = jnp.sum(two * place, axis=0, keepdims=True)
    meta[plane, 2:4] = routing_ref[...]

    def tell(to):
        return remote(
            meta.at[plane],
            meta.at[plane],
            send_meta.at[to],
            recv_meta.at[plane],
            {"sp": to * members + member},
        )

    def told(source):
        return remote(
            meta.at[source],
            meta.at[source],
            send_meta.at[source],
            recv_meta.at[source],
            {"sp": source * members + member},
        )

    def part_of(c):
        return pl.ds(pl.multiple_of(c * chunk, chunk), chunk)

    def along(source, c, up):
        piece = gathered.at[source, part_of(c)]
        return remote(
            piece,
            piece,
            send_line.at[2 * source + up, c],
            recv_line.at[source, c],
            {"sp": me + (2 * up - 1) * members},
        )

    def along_own(c, up):
        return remote(
            normed_ref.at[part_of(c)],
            gathered.at[plane, part_of(c)],
            send_line.at[2 * plane + up, c],
            recv_line.at[plane, c],
            {"sp": me + (2 * up - 1) * members},
        )

    def arrive(source, c):
        along(source, c, 0).wait_recv()

        @pl.when(inner & (source < plane))
        def _():
            along(source, c, 1).start()

        @pl.when(inner & (source > plane))
        def _():
            along(source, c, 0).start()

    def outward(source, to):
        return remote(
            picked.at[source, to],
            rows_in.at[source, 0, member],
            send_pick.at[source, to],
            recv_pick.at[source, member],
            {"sp": plane * members + to},
        )

    def inward(source, origin):
        return remote(
            picked.at[source, origin],
            rows_in.at[source, 0, origin],
            send_pick.at[source, origin],
            recv_pick.at[source, origin],
            {"sp": plane * members + origin},
        )

    def stay(source):
        return pltpu.make_async_copy(
            picked.at[source, member], rows_in.at[source, 0, member], copy_pick.at[source]
        )

    def sharing(source):
        return remote(
            rows_in.at[source, 0],
            rows_in.at[source, 1],
            send_share.at[source],
            recv_share.at[source],
            peer,
        )

    def trading(source):
        return remote(
            given.at[source], taken.at[source], send_part.at[source], recv_part.at[source], peer
        )

    def homeward(source, to):
        target = source * members + to
        return remote(
            summed.at[source, to],
            returned.at[me],
            send_back.at[target],
            recv_back.at[me],
            {"sp": target},
        )

    def homecoming(origin):
        return remote(
            summed.at[0, 0],
            returned.at[origin],
            send_back.at[origin],
            recv_back.at[origin],
            {"sp": origin},
        )

    def dispatch(source):
        slot = lax.broadcasted_iota(jnp.int32, (slots, rows), 0) + plane * slots
        slot = slot.astype(jnp.float32)
        table = meta[source]
        wanted = ((slot == table[0:1]) | (slot == table[1:2])).astype(jnp.bfloat16)

        def some(i):
            values = product(wanted, gathered[source, :, columns_of(i)]).astype(jnp.bfloat16)
            picked[source, :, :, columns_of(i)] = values.reshape(members, capacity, COLUMNS)

        repeat(0, parts, some)
        repeat(1, members, lambda q: outward(source, lax.rem(member + q, members)).start())
        stay(source).start()

    def share(source):
        repeat(1, members, lambda q: inward(source, lax.rem(member + q, members)).wait_recv())
        stay(source).wait()
        sharing(source).start()

    def compute(source):
        sharing(source).wait_recv()
        values = rows_in[source].reshape(2 * slots, width)
        gate = product(values, gate_ref[...])
        up = product(values, up_ref[...])
        hidden = (jax.nn.silu(gate) * up).astype(jnp.bfloat16)
        part = product(hidden, down_ref[...]).astype(jnp.bfloat16)
        part = part.reshape(2, members, capacity, width)
        given[source] = part[1]
        kept[source] = part[0]
        trading(source).start()

    def home(source):
        trading(source).wait_recv()
        summed[source] = (
            kept[source].astype(jnp.float32) + taken[source].astype(jnp.float32)
        ).astype(jnp.bfloat16)

        def start(q):
            to = lax.rem(member + q, members)

            @pl.when((source != plane) | (q > 0))
            def _():
                homeward(source, to).start()

        repeat(0, members, start)

    pl.semaphore_wait(barrier, PLANES - 1 + members)
    for off in range(1, PLANES):
        tell(lax.rem(plane + off, PLANES)).start()
    for c in range(CHUNKS):

        @pl.when(plane < PLANES - 1)
        def _():
            along_own(c, 1).start()

        @pl.when(plane > 0)
        def _():
            along_own(c, 0).start()

    own.wait()
    dispatch(plane)
    for load in loads[:3]:
        load.wait()
    gate = product(normed_ref[...], common_gate[...])
    up = product(normed_ref[...], common_up[...])
    hidden = (jax.nn.silu(gate) * up).astype(jnp.bfloat16)

    def shared(i):
        feed[:, columns_of(i)] = normed_ref[:, columns_of(i)].astype(jnp.float32) + product(
            hidden, common_down[:, columns_of(i)]
        )

    repeat(0, parts, shared)
    for off in range(1, PLANES):
        told(lax.rem(plane + off, PLANES)).wait_recv()

    @pl.when(inner)
    def _():
        arrive(source_at(1), 0)
        arrive(source_at(2), 0)

    share(plane)
    for load in loads[3:]:
        load.wait()

    def step(k):
        source, following = source_at(k), source_at(k + 1)
        more = k < PLANES - 1

        @pl.when(inner & (k == 0))
        def _():
            arrive(source_at(1), 1)
            arrive(source_at(2), 1)

        @pl.when(inner & (k > 0) & more)
        def _():
            arrive(source_at(3), k - 1)

        @pl.when(jnp.logical_not(inner) & more)
        def _():
            for c in range(CHUNKS):
                arrive(following, c)

        @pl.when(more)
        def _():
            dispatch(following)

        compute(source)
        home(source)

        @pl.when(more)
        def _():
            share(following)

    repeat(0, PLANES, step)
    returned[me] = summed[plane, member]

    def combine(k):
        source = source_at(k)

        def come(q):
            origin = source * members + lax.rem(member + q, members)

            @pl.when(origin != me)
            def _():
                homecoming(origin).wait_recv()

        repeat(0, members, come)
        slot = lax.broadcasted_iota(jnp.int32, (slots, rows), 0) + source * slots
        slot = slot.astype(jnp.float32)
        table = meta[plane]
        share_of = jnp.where(slot == table[0:1], table[2:3], 0.0)
        share_of = share_of + jnp.where(slot == table[1:2], table[3:4], 0.0)
        high = share_of.astype(jnp.bfloat16)
        low = (share_of - high.astype(jnp.float32)).astype(jnp.bfloat16)
        begin = pl.multiple_of(source * members, members)

        def some(i):
            values = returned[pl.ds(begin, members), :, columns_of(i)].reshape(slots, COLUMNS)
            feed[:, columns_of(i)] += product(high, values, OVER) + product(low, values, OVER)

        repeat(0, parts, some)

    repeat(0, PLANES, combine)

    def normalize(i):
        some = pl.ds(pl.multiple_of(i * NORM_ROWS, NORM_ROWS), NORM_ROWS)
        out_ref[some] = layer_norm(feed[some], gain_ref[...]).astype(jnp.bfloat16)

    repeat(0, rows // NORM_ROWS, normalize)

    for off in range(1, PLANES):
        tell(lax.rem(plane + off, PLANES)).wait_send()
    for c in range(CHUNKS):

        @pl.when(plane < PLANES - 1)
        def _():
            along_own(c, 1).wait_send()

        @pl.when(plane > 0)
        def _():
            along_own(c, 0).wait_send()

        for source in range(PLANES):

            @pl.when(inner & (source < plane))
            def _():
                along(source, c, 1).wait_send()

            @pl.when(inner & (source > plane))
            def _():
                along(source, c, 0).wait_send()

    def sent(source):
        repeat(1, members, lambda q: outward(source, lax.rem(member + q, members)).wait_send())
        sharing(source).wait_send()
        trading(source).wait_send()

        def gone(q):
            to = lax.rem(member + q, members)

            @pl.when((source != plane) | (q > 0))
            def _():
                homeward(source, to).wait_send()

        repeat(0, members, gone)

    repeat(0, PLANES, sent)


def experts(normed, routes, routing, gain, capacity, weights):
    n = lax.axis_size("sp")
    rows, width = normed.shape
    members = n // PLANES
    kind = normed.dtype
    group = (PLANES, members, capacity, width)
    vmem, anywhere = pl.BlockSpec(memory_space=pltpu.VMEM), pl.BlockSpec(memory_space=pl.ANY)

    def dma(*shape):
        return pltpu.SemaphoreType.DMA(shape)

    return pl.pallas_call(
        functools.partial(expert_kernel, n),
        in_specs=[vmem] * 4 + [anywhere] * 6,
        out_specs=vmem,
        out_shape=jax.ShapeDtypeStruct(normed.shape, kind),
        scratch_shapes=[pltpu.VMEM(w.shape, w.dtype) for w in weights]
        + [
            pltpu.VMEM((PLANES, 8, rows), jnp.float32),
            pltpu.VMEM((PLANES, rows, width), kind),
            pltpu.VMEM(group, kind),
            pltpu.VMEM((PLANES, 2) + group[1:], kind),
            pltpu.VMEM(group, kind),
            pltpu.VMEM(group, kind),
            pltpu.VMEM(group, kind),
            pltpu.VMEM(group, kind),
            pltpu.VMEM((n, capacity, width), kind),
            pltpu.VMEM((rows, width), jnp.float32),
            dma(7),
            dma(PLANES),
            dma(PLANES),
            dma(2 * PLANES, CHUNKS),
            dma(PLANES, CHUNKS),
            dma(PLANES, members),
            dma(PLANES, members),
            dma(PLANES),
            dma(PLANES),
            dma(PLANES),
            dma(PLANES),
            dma(PLANES),
            dma(n),
            dma(n),
        ],
        compiler_params=pltpu.CompilerParams(collective_id=1, has_side_effects=True),
        name="experts",
    )(normed, routes, routing, gain, *weights)


def per_device(
    query_matrix,
    key_matrix,
    value_matrix,
    output_gate_logits,
    decay_preactivation,
    head_extra_decay,
    residual,
    head_norm_gain,
    output_projection_weight,
    mixer_norm_gain,
    routes,
    routing_weight,
    routed_gate_weight,
    routed_up_weight,
    routed_down_weight,
    common_gate_weight,
    common_up_weight,
    common_down_weight,
    final_norm_gain,
):
    gain = jnp.concatenate([head_norm_gain] * (LANES // KEY_HEAD_SIZE))[None]
    normed = mixer(
        query_matrix,
        key_matrix,
        value_matrix,
        output_gate_logits,
        decay_preactivation,
        head_extra_decay.T,
        residual,
        gain,
        mixer_norm_gain[None],
        output_projection_weight,
    )
    row_count, top_count = routes.shape
    capacity = max(2, row_count * top_count // lax.axis_size("sp") * 2)
    return experts(
        normed,
        routes.T,
        routing_weight.T,
        final_norm_gain[None],
        capacity,
        (
            routed_gate_weight[0],
            routed_up_weight[0],
            routed_down_weight[0],
            common_gate_weight,
            common_up_weight,
            common_down_weight,
        ),
    )


def solution(mesh):
    placed = (
        P("sp", "tp"),
        P("sp", "tp"),
        P("sp", "tp"),
        P("sp", "tp"),
        P("sp", "tp"),
        P("sp", "tp"),
        P(("sp", "tp"), None),
        P(),
        P("tp", None),
        P(),
        P(("sp", "tp"), None),
        P(("sp", "tp"), None),
        P("sp", None, "tp"),
        P("sp", None, "tp"),
        P("sp", "tp", None),
        P(),
        P(),
        P(),
        P(),
    )
    return jax.shard_map(
        per_device, mesh=mesh, in_specs=placed, out_specs=P(("sp", "tp"), None), check_vma=False
    )
```
